32 devices in a mesh: sp: 16 (over z, y, x), tp: 2 (over core).
Axes of the slice: x: 2, y: 2, z: 4, core: 2. Of those that a mesh axis runs over, the one named last changes fastest.
Arguments:
- tokens: bfloat16 [1536, 4, 1024], P(('sp', 'tp')), may hold values from -6 to 6
- in_gain: float32 [1024], replicated, may hold values from 0.1 to 1.9
- w_query: bfloat16 [1024, 1024], P('sp', 'tp'), may hold values from -0.1875 to 0.1875
- w_key: bfloat16 [1024, 1024], P('sp', 'tp'), may hold values from -0.1875 to 0.1875
- w_value: bfloat16 [1024, 1024], P('sp', 'tp'), may hold values from -0.1875 to 0.1875
- w_gate: bfloat16 [1024, 1024], P('sp', 'tp'), may hold values from -0.1875 to 0.1875
- w_beta: bfloat16 [1024, 8], P('sp', 'tp'), may hold values from -0.1875 to 0.1875
- conv_query: bfloat16 [4, 1024], P(None, 'tp'), may hold values from -3 to 3
- conv_key: bfloat16 [4, 1024], P(None, 'tp'), may hold values from -3 to 3
- conv_value: bfloat16 [4, 1024], P(None, 'tp'), may hold values from -3 to 3
- decay_rate: float32 [8], P('tp'), may hold values from 0.1 to 3
- out_gain: float32 [128], replicated, may hold values from 0.1 to 1.9
- w_out: bfloat16 [1024, 1024], P('tp', 'sp'), may hold values from -0.1875 to 0.1875
Outputs:
- mixed: bfloat16 [1536, 4, 1024], P(('sp', 'tp'))
The draws below stay inside these ranges and needn't reach their ends.
All inputs are finite; a program needn't handle non-finite values.
Results may differ from the reference program's by a relative error of at most 0.02.
Values may be sent and summed in bfloat16 or wider, within the bound.
A program may use at most 64 MiB of HBM per device.

```python
import math
import jax
import jax.numpy as jnp
from jax import lax

D = 1024
HEADS = 8
DK = 128
CONV_K = 4
BLOCK = 32
SEQS = 4
TOKENS = 1536


def shard_levels(own_key, extent, shards, low, top_value):
    level, own = 1.0, jax.random.fold_in(own_key, 6)
    for dim, parts in shards:
        heights = jnp.exp(jax.random.uniform(jax.random.fold_in(own, dim), (parts,), jnp.float32, low / len(shards), top_value / len(shards)))
        level = level * jnp.repeat(heights, extent[dim] // parts).reshape([-1 if axis == dim else 1 for axis in range(len(extent))])
    return level


def normal_values(stream_key, shape, spread, limit, shards=(), held_as=jnp.bfloat16):
    values = spread * jax.random.normal(stream_key, shape, jnp.float32)
    if shards:
        values = values * shard_levels(stream_key, shape, shards, -0.22, 0.18)
    return jnp.clip(values, -limit, limit).astype(held_as)


def setup_inputs(seed: int = 0) -> dict:
    key_of = jax.random.split(jax.random.key(seed), 14)
    tokens = normal_values(key_of[0], (TOKENS, SEQS, D), 1.0, 6.0, ((0, 32),))
    in_gain = jnp.clip(1.0 + 0.18 * jax.random.normal(key_of[1], (D,), jnp.float32), 0.1, 1.9)
    w_query = normal_values(key_of[2], (D, HEADS * DK), D ** -0.5, 0.1875, ((0, 16), (1, 2)))
    w_key = normal_values(key_of[3], (D, HEADS * DK), D ** -0.5, 0.1875, ((0, 16), (1, 2)))
    w_value = normal_values(key_of[4], (D, HEADS * DK), D ** -0.5, 0.1875, ((0, 16), (1, 2)))
    w_gate = normal_values(key_of[5], (D, HEADS * DK), D ** -0.5, 0.1875, ((0, 16), (1, 2)))
    w_beta = normal_values(key_of[6], (D, HEADS), D ** -0.5, 0.1875, ((0, 16), (1, 2)))
    conv_query = normal_values(key_of[7], (CONV_K, HEADS * DK), CONV_K ** -0.5, 3.0, ((1, 2),))
    conv_key = normal_values(key_of[8], (CONV_K, HEADS * DK), CONV_K ** -0.5, 3.0, ((1, 2),))
    conv_value = normal_values(key_of[9], (CONV_K, HEADS * DK), CONV_K ** -0.5, 3.0, ((1, 2),))
    decay_rate = jnp.clip(jnp.exp(math.log(3.0) - 3.4011974 * jax.random.uniform(key_of[10], (HEADS,), jnp.float32) ** shard_levels(key_of[10], (HEADS,), ((0, 2),), -0.2, 0.2)), 0.1, 3.0)
    out_gain = jnp.clip(1.0 + 0.18 * jax.random.normal(key_of[11], (DK,), jnp.float32), 0.1, 1.9)
    w_out = normal_values(key_of[12], (HEADS * DK, D), (HEADS * DK) ** -0.5, 0.1875, ((0, 2), (1, 16)))
    return {"tokens": tokens, "in_gain": in_gain, "w_query": w_query, "w_key": w_key, "w_value": w_value, "w_gate": w_gate, "w_beta": w_beta, "conv_query": conv_query, "conv_key": conv_key, "conv_value": conv_value, "decay_rate": decay_rate, "out_gain": out_gain, "w_out": w_out}


epsilon = 1e-06
out_epsilon = 1e-10
highest = lax.Precision.HIGHEST

def unit_inverse(lower):
    size = lower.shape[-1]
    inverse = jnp.eye(size, dtype=jnp.float32) - lower
    power = jnp.matmul(lower, lower, precision=highest)
    span = 2
    while span < size:
        inverse = inverse + jnp.matmul(inverse, power, precision=highest)
        power = jnp.matmul(power, power, precision=highest)
        span = span * 2
    return inverse

def make_terms(query, keys, values, beta, rate_col):
    size = query.shape[-2]
    steps = jnp.arange(1, size + 1).astype(jnp.float32)
    cumulative = -rate_col * steps
    lower_mask = jnp.tril(jnp.ones((size, size), bool))
    strict_mask = jnp.tril(jnp.ones((size, size), bool), -1)
    decay = jnp.where(lower_mask, jnp.exp(cumulative[..., :, None] - cumulative[..., None, :]), 0.0)
    weighted = keys * beta[..., None]
    lower = jnp.where(strict_mask, jnp.einsum('...cd,...sd->...cs', weighted, keys, precision=highest) * decay, 0.0)
    inverse = unit_inverse(lower)
    update = jnp.einsum('...cs,...sv->...cv', inverse, values * beta[..., None], precision=highest)
    erase = jnp.einsum('...cs,...sd->...cd', inverse, weighted * jnp.exp(cumulative)[..., None], precision=highest)
    scores = jnp.einsum('...cd,...sd->...cs', query, keys, precision=highest) * decay
    query_decayed = query * jnp.exp(cumulative)[..., None]
    final = cumulative[..., -1:]
    keys_decayed = keys * jnp.exp(final - cumulative)[..., None]
    return (query_decayed, keys_decayed, update, erase, scores, jnp.exp(final))

def apply_block(state, terms):
    query_decayed, keys_decayed, update, erase, scores, kept = terms
    fresh = update - jnp.einsum('...cd,...dv->...cv', erase, state, precision=highest)
    output = jnp.einsum('...cd,...dv->...cv', query_decayed, state, precision=highest)
    output = output + jnp.einsum('...cs,...sv->...cv', scores, fresh, precision=highest)
    state = state * kept[..., None] + jnp.einsum('...cd,...cv->...dv', keys_decayed, fresh, precision=highest)
    return (state, output)

def causal_conv(pre, conv_taps, history):
    width = conv_taps.shape[0]
    extended = jnp.concatenate([history, pre], axis=0).astype(jnp.float32)
    length = pre.shape[0]
    total = jnp.zeros(pre.shape, jnp.float32)
    for tap in range(width):
        total = total + extended[tap:tap + length] * conv_taps[tap].astype(jnp.float32)
    return total

def rms_scale(values_in, gain):
    values = values_in.astype(jnp.float32)
    scaled = values * lax.rsqrt(lax.optimization_barrier(jnp.mean(values * values, axis=-1, keepdims=True)) + epsilon)
    return (scaled * gain).astype(jnp.bfloat16)

def l2_normalize(array):
    return array * lax.rsqrt(lax.optimization_barrier(jnp.sum(array * array, axis=-1, keepdims=True)) + epsilon)

def finish(outputs, out_gain, gate_pre):
    normed = outputs * lax.rsqrt(lax.optimization_barrier(jnp.mean(outputs * outputs, axis=-1, keepdims=True)) + out_epsilon) * out_gain
    gate = jax.nn.silu(gate_pre.astype(jnp.float32)).reshape(outputs.shape)
    return (normed * gate).astype(jnp.bfloat16).reshape(outputs.shape[0], outputs.shape[1], -1)

def reference(tokens, in_gain, w_query, w_key, w_value, w_gate, w_beta, conv_query, conv_key, conv_value, decay_rate, out_gain, w_out):
    width = tokens.shape[2]
    head_width = HEADS * DK
    normed = rms_scale(tokens, in_gain)
    flat = normed.reshape(-1, width)

    def project(weight):
        return jnp.dot(flat, weight, preferred_element_type=jnp.float32).astype(jnp.bfloat16).reshape(TOKENS, SEQS, -1)
    mixed_pre = jnp.concatenate([project(w_query), project(w_key), project(w_value)], axis=2)
    gate_pre = project(w_gate)
    beta_pre = project(w_beta)
    history = jnp.zeros((CONV_K - 1, SEQS, 3 * head_width), jnp.bfloat16)
    conv_taps = jnp.concatenate([conv_query, conv_key, conv_value], axis=1)
    convolved = jax.nn.silu(causal_conv(mixed_pre, conv_taps, history))

    def split_heads(array):
        return array.reshape(TOKENS, SEQS, HEADS, DK)
    query = l2_normalize(split_heads(convolved[:, :, :head_width])) * DK ** (-0.5)
    keys = l2_normalize(split_heads(convolved[:, :, head_width:2 * head_width]))
    values = split_heads(convolved[:, :, 2 * head_width:])
    beta = jax.nn.sigmoid(beta_pre.astype(jnp.float32) + math.log(DK / (4.0 * TOKENS)))
    rate_col = (decay_rate / TOKENS)[:, None]
    blocks = TOKENS // BLOCK

    def to_blocks(array):
        return jnp.moveaxis(array.reshape(blocks, BLOCK, SEQS, HEADS, DK), 1, 3)
    beta_blocks = jnp.moveaxis(beta.reshape(blocks, BLOCK, SEQS, HEADS), 1, 3)

    def advance(state, inputs):
        query_block, key_block, value_block, beta_block = inputs
        return apply_block(state, make_terms(query_block, key_block, value_block, beta_block, rate_col))
    initial = jnp.zeros((SEQS, HEADS, DK, DK), jnp.float32)
    _, outputs = lax.scan(advance, initial, (to_blocks(query), to_blocks(keys), to_blocks(values), beta_blocks))
    outputs = jnp.moveaxis(outputs, 3, 1).reshape(TOKENS, SEQS, HEADS, DK)
    gated = finish(outputs, out_gain, gate_pre)
    mixed = jnp.dot(gated.reshape(-1, head_width), w_out, preferred_element_type=jnp.float32).astype(jnp.bfloat16)
    return mixed.reshape(TOKENS, SEQS, width)
```

```python
import functools
import math

import jax
import jax.numpy as jnp
from jax import lax
from jax.experimental import pallas as pl
from jax.experimental.pallas import tpu as pltpu
from jax.sharding import PartitionSpec as P

PAD = 16
LANES = 128
epsilon = 1e-06
out_epsilon = 1e-10
f32 = jnp.float32
bf16 = jnp.bfloat16
NN, NT, TN = ((1,), (0,)), ((1,), (1,)), ((0,), (0,))


def dot(a, b, dims=NN):
    return lax.dot_general(
        a.astype(bf16), b.astype(bf16), (dims, ((), ())), preferred_element_type=f32
    )


def rms_scale(values_in, gain):
    values = values_in.astype(f32)
    scaled = values * lax.rsqrt(jnp.mean(values * values, axis=-1, keepdims=True) + epsilon)
    return (scaled * gain).astype(bf16)


def l2_normalize(array):
    return array * lax.rsqrt(jnp.sum(array * array, axis=-1, keepdims=True) + epsilon)


def unit_inverse(lower, row, col):
    size = lower.shape[0]
    near = ((row >> 1) == (col >> 1)) & (row != col)
    inverse = jnp.where(row == col, 1.0, 0.0) - jnp.where(near, lower, 0.0)
    level = 1
    while (1 << level) < size:
        mask = ((row >> (level + 1)) == (col >> (level + 1))) & ((row >> level) != (col >> level))
        cross = jnp.where(mask, lower, 0.0)
        inverse = inverse - dot(inverse, dot(cross, inverse))
        level += 1
    return inverse


def pair_terms(block, beta, taps, rate, depth):
    width = taps[0].shape[0]
    size = beta.shape[0]

    def conv(part):
        x = block[part].astype(f32)
        total = x * taps[part][width - 1 : width]
        for back in range(1, width):
            total = total + pltpu.roll(x, back, 0) * taps[part][width - 1 - back : width - back]
        total = total[PAD:]
        return total * jax.nn.sigmoid(total)

    query = l2_normalize(conv(0)) * depth ** (-0.5)
    keys = l2_normalize(conv(1))
    values = conv(2)
    row = lax.broadcasted_iota(jnp.int32, (size, size), 0)
    col = lax.broadcasted_iota(jnp.int32, (size, size), 1)
    decay = jnp.exp(-rate * jnp.maximum(row - col, 0).astype(f32))
    step = lax.broadcasted_iota(jnp.int32, (size, 1), 0).astype(f32)
    kept = jnp.exp(-rate * (step + 1.0))
    rest = jnp.exp(-rate * (size - 1.0 - step))
    weighted = keys * beta
    products = dot(jnp.concatenate([weighted, query], axis=0), keys, NT)
    lower = jnp.where(row > col, products[:size] * decay, 0.0)
    scores = jnp.where(row >= col, products[size:] * decay, 0.0)
    inverse = unit_inverse(lower, row, col)
    both = dot(inverse, jnp.concatenate([values * beta, weighted * kept], axis=1))
    seen = dot(scores, both)
    moved = dot(keys * rest, both, TN)
    return moved, query * kept - seen[:, depth:], seen[:, :depth]


def terms_kernel(heads, depth, shift, pre_ref, taps_ref, rate_ref, map_ref, read_ref, local_ref):
    head_width = heads * depth
    beta = jax.nn.sigmoid(pre_ref[0, PAD:, 4 * head_width :].astype(f32) + shift)
    for head in range(heads):
        places = [pl.ds(part * head_width + head * depth, depth) for part in range(3)]
        moved, read, local = pair_terms(
            [pre_ref[0, :, place] for place in places],
            beta[:, head : head + 1],
            [taps_ref[:, place] for place in places],
            rate_ref[head],
            depth,
        )
        map_ref[0, head] = moved.astype(bf16)
        read_ref[0, head] = read.astype(bf16)
        local_ref[0, head] = local


def chain_kernel(depth, kept_ref, map_ref, state_ref):
    state = jnp.zeros((depth, depth), f32)
    for index in range(map_ref.shape[0]):
        state_ref[index] = state.astype(bf16)
        state = (
            state * kept_ref[0]
            + map_ref[index, :, :depth].astype(f32)
            - dot(map_ref[index, :, depth:], state)
        )


def finish_kernel(heads, depth, read_ref, local_ref, state_ref, pre_ref, gain_ref, gated_ref):
    for head in range(heads):
        out = local_ref[0, head] + dot(read_ref[0, head], state_ref[0, head])
        out = out * lax.rsqrt(jnp.mean(out * out, axis=-1, keepdims=True) + out_epsilon)
        place = pl.ds(head * depth, depth)
        gate = pre_ref[0, PAD:, place].astype(f32)
        gate = gate * jax.nn.sigmoid(gate)
        gated_ref[0, :, place] = (out * gain_ref[...] * gate).astype(bf16)


def incoming_states(maps, kept):
    pairs, depth, _ = maps.shape
    length, here = lax.axis_size("sp"), lax.axis_index("sp")
    if pairs == length:
        mine = lax.all_to_all(maps, "sp", 0, 0, tiled=True)
        states = pl.pallas_call(
            functools.partial(chain_kernel, depth),
            out_shape=jax.ShapeDtypeStruct((length, depth, depth), bf16),
            in_specs=[
                pl.BlockSpec(memory_space=pltpu.SMEM),
                pl.BlockSpec(memory_space=pltpu.VMEM),
            ],
            out_specs=pl.BlockSpec(memory_space=pltpu.VMEM),
        )(lax.dynamic_slice_in_dim(kept, here, 1, 0), mine)
        return lax.all_to_all(states, "sp", 0, 0, tiled=True)
    everything = lax.all_gather(maps, "sp")

    def hop(index, state):
        moved = everything[index].astype(f32)
        erased = jnp.einsum(
            "pde,pev->pdv",
            moved[:, :, depth:].astype(bf16),
            state.astype(bf16),
            preferred_element_type=f32,
        )
        new = state * kept[:, None, None] + moved[:, :, :depth] - erased
        return jnp.where(index < here, new, state)

    state = lax.fori_loop(0, length, hop, jnp.zeros((pairs, depth, depth), f32))
    return state.astype(bf16)


def body(
    tokens,
    in_gain,
    w_query,
    w_key,
    w_value,
    w_gate,
    w_beta,
    conv_query,
    conv_key,
    conv_value,
    decay_rate,
    out_gain,
    w_out,
):
    seqs, width = tokens.shape[1], tokens.shape[2]
    head_width = w_query.shape[1]
    heads = w_beta.shape[1]
    depth = head_width // heads
    taps = conv_query.shape[0]
    length = lax.axis_size("sp")

    beta_pad = jnp.pad(w_beta, ((0, 0), (0, LANES - heads)))
    packed = jnp.concatenate([w_query, w_key, w_value, w_gate, beta_pad], axis=1)
    weights = lax.all_gather(packed, "sp", axis=0, tiled=True)
    full_out = lax.all_gather(w_out.T, "sp", axis=0, tiled=True)

    normed = jnp.swapaxes(rms_scale(tokens, in_gain), 0, 1)
    normed = lax.all_gather(normed, "tp", axis=1, tiled=True)
    span = normed.shape[1]
    history = lax.ppermute(
        normed[:, span - taps + 1 :], "sp", [(i, i + 1) for i in range(length - 1)]
    )
    filler = jnp.zeros((seqs, PAD - taps + 1, width), bf16)
    extended = jnp.concatenate([filler, history, normed], axis=1)
    rows = PAD + span
    pre = jnp.dot(
        extended.reshape(-1, width), weights, preferred_element_type=f32
    ).astype(bf16)
    pre = pre.reshape(seqs, rows, -1)

    total_tokens = span * length
    rate = decay_rate / total_tokens
    shift = math.log(depth / (4.0 * total_tokens))
    conv_taps = jnp.concatenate([conv_query, conv_key, conv_value], axis=1).astype(f32)

    def per_seq(*shape):
        return pl.BlockSpec((1,) + shape, lambda s: (s,) + (0,) * len(shape))

    maps, reads, locals_ = pl.pallas_call(
        functools.partial(terms_kernel, heads, depth, shift),
        grid=(seqs,),
        in_specs=[
            per_seq(rows, pre.shape[2]),
            pl.BlockSpec(conv_taps.shape, lambda s: (0, 0)),
            pl.BlockSpec(memory_space=pltpu.SMEM),
        ],
        out_specs=[
            per_seq(heads, depth, 2 * depth),
            per_seq(heads, span, depth),
            per_seq(heads, span, depth),
        ],
        out_shape=[
            jax.ShapeDtypeStruct((seqs, heads, depth, 2 * depth), bf16),
            jax.ShapeDtypeStruct((seqs, heads, span, depth), bf16),
            jax.ShapeDtypeStruct((seqs, heads, span, depth), f32),
        ],
    )(pre, conv_taps, rate)

    kept = jnp.tile(jnp.exp(-rate * span), seqs)
    states = incoming_states(maps.reshape(seqs * heads, depth, 2 * depth), kept)
    gated = pl.pallas_call(
        functools.partial(finish_kernel, heads, depth),
        grid=(seqs,),
        in_specs=[
            per_seq(heads, span, depth),
            per_seq(heads, span, depth),
            per_seq(heads, depth, depth),
            pl.BlockSpec((1, rows, head_width), lambda s: (s, 0, 3)),
            pl.BlockSpec((1, depth), lambda s: (0, 0)),
        ],
        out_specs=per_seq(span, head_width),
        out_shape=jax.ShapeDtypeStruct((seqs, span, head_width), bf16),
    )(reads, locals_, states.reshape(seqs, heads, depth, depth), pre, out_gain[None])

    mixed = lax.dot_general(
        gated, full_out, (((2,), (1,)), ((), ())), preferred_element_type=f32
    ).astype(bf16)
    mixed = lax.psum_scatter(mixed, "tp", scatter_dimension=1, tiled=True)
    return jnp.swapaxes(mixed, 0, 1)


def solution(mesh):
    placed = (
        P(("sp", "tp"), None, None),
        P(),
        P("sp", "tp"),
        P("sp", "tp"),
        P("sp", "tp"),
        P("sp", "tp"),
        P("sp", "tp"),
        P(None, "tp"),
        P(None, "tp"),
        P(None, "tp"),
        P("tp"),
        P(),
        P("tp", "sp"),
    )
    return jax.shard_map(
        body, mesh=mesh, in_specs=placed, out_specs=P(("sp", "tp"), None, None), check_vma=False
    )
```
